512 devices in a mesh: grp: 2 (over y), fs: 64 (over z, core), tp: 4 (over x).
Axes of the slice: x: 4, y: 2, z: 32, core: 2. Of those that a mesh axis runs over, the one named last changes fastest.
The devices are a block of a 4x8x32 slice.
Arguments:
- tokens: bfloat16 [16384, 2048], P(('grp', 'fs'), 'tp'), parts along dimension 0, may hold values from -300 to 300
- routes: int32 [16384, 8], P(('grp', 'fs')), parts along dimension 0, may hold values from 0 to 63, all different within a row; in each aligned block of 128 rows (0 to 127, 128 to 255, ...) at most 32 rows name the same one
- route_scores: float32 [16384, 8], P(('grp', 'fs')), parts along dimension 0, may hold values from 0.05 to 1
- norm_gain: float32 [2048], P('fs'), may hold values from 0.1 to 1.9
- expert_gate: float32 [64, 2048, 256], P(None, 'fs', 'tp'), may hold values from -6 to 6
- expert_up: float32 [64, 2048, 256], P(None, 'fs', 'tp'), may hold values from -6 to 6
- expert_down: float32 [64, 2048, 256], P(None, 'fs', 'tp'), may hold values from -6 to 6
- shared_gate: float32 [2048, 256], P('fs', 'tp'), may hold values from -6 to 6
- shared_up: float32 [2048, 256], P('fs', 'tp'), may hold values from -6 to 6
- shared_down: float32 [2048, 256], P('fs', 'tp'), may hold values from -6 to 6
Outputs:
- served_gate: bfloat16 [128, 2048, 256], P(('grp', 'fs'), 'tp'), parts along dimension 0
- served_up: bfloat16 [128, 2048, 256], P(('grp', 'fs'), 'tp'), parts along dimension 0
- served_down: bfloat16 [128, 2048, 256], P(('grp', 'fs'), 'tp'), parts along dimension 0
- common_gate: bfloat16 [4096, 256], P(('grp', 'tp')), parts along dimension 0
- common_up: bfloat16 [4096, 256], P(('grp', 'tp')), parts along dimension 0
- common_down: bfloat16 [4096, 256], P(('grp', 'tp')), parts along dimension 0
- mixture: bfloat16 [16384, 2048], P(('grp', 'fs'), 'tp'), parts along dimension 0
The draws below stay inside these ranges and needn't reach their ends.
There are 2 independent parts, one for each index of `grp`. The reference program is written for one: setup_inputs(seed, part) draws one part's arguments, and reference() takes and returns one part's arrays. A program takes and returns all parts, laid end to end along the dimension named above; an argument that names none is the same for every part. Nothing has to cross between parts.
Inputs may be any that keep to these rules, and one draw needn't show every extreme that they name: `routes`: each row names 8 different experts. Within the rows of one index of fs (aligned blocks of 128 rows) no expert is named by more than 32 rows, a bound that some block reaches.
All inputs are finite; a program needn't handle non-finite values.
Results may differ from the reference program's by a relative error of at most 0.018.
Values may be sent and summed in bfloat16 or wider, within the bound.
No kernel may reach another device: no remote copies, remote signals or barrier semaphores. Data moves between devices by JAX's collectives and lax.ppermute only.
A program may use at most 64 MiB of HBM per device.

```python
import math
import jax
import jax.numpy as jnp
import numpy as np
from jax import lax

D = 2048
H = 256
SH = 256
TOK_DEV = 128
TOKENS = 8192
EXPERTS = 64
TOP_K = 8
CAP = 32
N_FS = 64
N_TP = 4


def draw_tokens(key, part):
    base_key = jax.random.fold_in(key, 11)
    subkeys = jax.random.split(base_key, 2)
    column_scale = jnp.exp(math.log(3.0) * jnp.arange(D, dtype=jnp.float32) / D)
    column_scale = column_scale * jax.random.uniform(subkeys[1], (D,), jnp.float32, 0.5, 1.5)
    values = jnp.clip(jax.random.normal(subkeys[0], (TOKENS, D), jnp.float32), -6.0, 6.0)
    return (values * column_scale[None, :]).astype(jnp.bfloat16)


def block_scale(key, shape, cuts, least, high):
    factor_of, own = 1.0, jax.random.fold_in(key, 6)
    for position, parts in cuts:
        heights = jnp.exp(jax.random.uniform(jax.random.fold_in(own, position), (parts,), jnp.float32, least / len(cuts), high / len(cuts)))
        factor_of = factor_of * jnp.repeat(heights, shape[position] // parts).reshape([-1 if axis == position else 1 for axis in range(len(shape))])
    return factor_of


def assign_block(stream_key, own, number, rows, count, top, most, skew):
    ranking = jax.random.permutation(stream_key, count)
    heavy_load, ordinary = portions_of(count, rows * top, most, skew, True), portions_of(count, rows * top, most, skew, False)
    places = jnp.arange(count)

    def named(lengths, turn):
        used = int((lengths > 0).sum())
        fixed = max(1, used // 4)
        passed = fixed + (places - fixed + turn * (used - fixed)) % max(1, count - fixed)
        return jnp.zeros((count,), jnp.int32).at[ranking[jnp.where(places < fixed, places, passed)]].set(jnp.asarray(lengths, jnp.int32))

    lengths = jnp.where(number % 4 == 0, named(heavy_load, number // 4), named(ordinary, number - number // 4 - 1))
    mixed = jax.random.permutation(jax.random.fold_in(own, 3), count)
    donor, sink = mixed[0:count // 2 * 2:2], mixed[1:count // 2 * 2:2]
    margin = jnp.minimum(lengths[donor] - 1, most - lengths[sink]) // 2
    margin = jnp.where((donor == ranking[0]) | (sink == ranking[0]) | (lengths[sink] == 0), 0, jnp.maximum(margin, 0))
    passed = jax.random.randint(jax.random.fold_in(own, 4), (count // 2,), 0, 1 << 20) % (margin + 1)
    lengths = lengths.at[donor].add(-passed).at[sink].add(passed)
    labels = jnp.searchsorted(jnp.cumsum(lengths), jnp.arange(rows * top), side="right").astype(jnp.int32)
    grid = labels.reshape(top, rows).T
    grid = grid[jax.random.permutation(jax.random.fold_in(own, 1), rows)]
    turn = jax.random.randint(jax.random.fold_in(own, 2), (rows, 1), 0, top)
    return jnp.take_along_axis(grid, (jnp.arange(top)[None, :] + turn) % top, axis=1)


def portions_of(count, total, bound, slope, full):
    portions = [(1 << 20) // math.isqrt(rank ** slope) + 1 for rank in range(1, count + 1)]
    largest = bound if full else min(bound, max(-(-total // count), total * portions[0] // sum(portions)))
    least = 1 if total - largest >= count - 1 else 0
    holding, spare = [largest] + [least] * (count - 1), total - largest - least * (count - 1)
    while spare > 0:
        candidates = [i for i in range(1, count) if holding[i] < largest] or [i for i in range(1, count) if holding[i] < bound]
        whole, remaining = sum([portions[i] for i in candidates]), spare
        for i in candidates:
            addition = min(bound - holding[i], max(1, remaining * portions[i] // whole), spare)
            holding[i] = holding[i] + addition
            spare = spare - addition
    return np.array(holding)


def centred(stream_key, shape, deviation, reach, cuts=(), kind=jnp.bfloat16):
    entries = deviation * jax.random.normal(stream_key, shape, jnp.float32)
    if cuts:
        entries = entries * block_scale(stream_key, shape, cuts, -0.22, 0.18)
    return jnp.clip(entries, -reach, reach).astype(kind)


def setup_inputs(seed: int = 0, part: int = 0) -> dict:
    key_of = jax.random.split(jax.random.key(seed), 11)
    part_keys = jax.random.split(jax.random.fold_in(key_of[10], part), 11)
    tokens = draw_tokens(jax.random.fold_in(jax.random.fold_in(key_of[10], part), 71), part)
    routes_keys = jax.random.split(jax.random.fold_in(part_keys[1], 1), TOKENS // TOK_DEV)
    routes_turns = jax.random.permutation(jax.random.fold_in(part_keys[1], 3), TOKENS // TOK_DEV)
    routes = jax.vmap(lambda own, number: assign_block(jax.random.fold_in(part_keys[1], 2), own, number, TOK_DEV, EXPERTS, TOP_K, CAP, 1))(routes_keys, routes_turns).reshape((TOKENS, TOP_K))
    route_scores = jnp.clip(0.05 + 0.95 * jax.random.uniform(part_keys[2], (TOKENS, TOP_K), jnp.float32) ** block_scale(part_keys[2], (TOKENS, TOP_K), ((0, 64),), -0.2, 0.2), 0.05, 1.0)
    norm_gain = jnp.clip(1.0 + 0.18 * jax.random.normal(key_of[3], (D,), jnp.float32), 0.1, 1.9)
    expert_gate = centred(key_of[4], (EXPERTS, D, H), 1.0, 6.0, ((1, 64), (2, 4)), jnp.float32)
    expert_up = centred(key_of[5], (EXPERTS, D, H), 1.0, 6.0, ((1, 64), (2, 4)), jnp.float32)
    expert_down = centred(key_of[6], (EXPERTS, D, H), 1.0, 6.0, ((1, 64), (2, 4)), jnp.float32)
    shared_gate = centred(key_of[7], (D, SH), 1.0, 6.0, ((0, 64), (1, 4)), jnp.float32)
    shared_up = centred(key_of[8], (D, SH), 1.0, 6.0, ((0, 64), (1, 4)), jnp.float32)
    shared_down = centred(key_of[9], (D, SH), 1.0, 6.0, ((0, 64), (1, 4)), jnp.float32)
    return {"tokens": tokens, "routes": routes, "route_scores": route_scores, "norm_gain": norm_gain, "expert_gate": expert_gate, "expert_up": expert_up, "expert_down": expert_down, "shared_gate": shared_gate, "shared_up": shared_up, "shared_down": shared_down}


EPSILON = 1e-05
ROUTED_SCALE = 2.5

def normalize(tokens):
    values = tokens.astype(jnp.float32)
    average = lax.optimization_barrier(jnp.mean(values, axis=1, keepdims=True))
    meansq = lax.optimization_barrier(jnp.mean(values * values, axis=1, keepdims=True))
    return ((values - average) * lax.rsqrt(meansq - average * average + EPSILON)).astype(jnp.bfloat16)

def gated_mlp(inputs, w_gate, w_up, w_down):
    model_width = inputs.shape[1]
    block_width = model_width // N_TP
    hidden_units = w_gate.shape[1]
    gate_total = jnp.zeros((inputs.shape[0], hidden_units), jnp.float32)
    up_total = jnp.zeros((inputs.shape[0], hidden_units), jnp.float32)
    for block_index in range(N_TP):
        low = block_index * block_width
        columns = inputs[:, low:low + block_width]
        gate_piece = jnp.dot(columns, w_gate[low:low + block_width], preferred_element_type=jnp.float32) * model_width ** (-0.5)
        up_piece = jnp.dot(columns, w_up[low:low + block_width], preferred_element_type=jnp.float32) * model_width ** (-0.5)
        gate_total = gate_total + gate_piece.astype(jnp.bfloat16).astype(jnp.float32)
        up_total = up_total + up_piece.astype(jnp.bfloat16).astype(jnp.float32)
    hidden = (jax.nn.silu(gate_total) * up_total).astype(jnp.bfloat16)
    return jnp.dot(hidden, w_down.T, preferred_element_type=jnp.float32) * hidden_units ** (-0.5)

def reference(tokens, routes, route_scores, norm_gain, expert_gate, expert_up, expert_down, shared_gate, shared_up, shared_down):
    gain_column = norm_gain[:, None]
    served_gate = (expert_gate * gain_column[None]).astype(jnp.bfloat16)
    served_up = (expert_up * gain_column[None]).astype(jnp.bfloat16)
    served_down = expert_down.astype(jnp.bfloat16)
    common_gate = (shared_gate * gain_column).astype(jnp.bfloat16)
    common_up = (shared_up * gain_column).astype(jnp.bfloat16)
    common_down = shared_down.astype(jnp.bfloat16)
    normed = normalize(tokens)
    mix_weight = route_scores / lax.optimization_barrier(jnp.sum(route_scores, axis=1, keepdims=True)) * ROUTED_SCALE
    running = gated_mlp(normed, common_gate, common_up, common_down)
    expert_ids = routes.reshape(-1).astype(jnp.int32)
    count_all = expert_ids.shape[0]
    sorted_order = jnp.argsort(expert_ids, stable=True).astype(jnp.int32)
    counts = jax.ops.segment_sum(jnp.ones_like(expert_ids), expert_ids, num_segments=EXPERTS)
    starts = jnp.cumsum(counts) - counts
    most_rows = N_FS * CAP
    flat_weights = mix_weight.reshape(-1)

    def one_expert(carried, expert_index):
        offsets = jnp.arange(most_rows, dtype=jnp.int32)
        picked = sorted_order[jnp.minimum(starts[expert_index] + offsets, count_all - 1)]
        live_rows = offsets < counts[expert_index]
        token_ids = picked // TOP_K
        expert_out = gated_mlp(normed[token_ids], served_gate[expert_index], served_up[expert_index], served_down[expert_index])
        expert_out = expert_out.astype(jnp.bfloat16).astype(jnp.float32)
        row_weight = jnp.where(live_rows, flat_weights[picked], jnp.zeros_like(flat_weights[picked]))
        return (carried.at[token_ids].add(expert_out * row_weight[:, None]), None)
    running, _ = lax.scan(one_expert, running, jnp.arange(EXPERTS, dtype=jnp.int32))
    mixture = running.astype(jnp.bfloat16)
    return (served_gate, served_up, served_down, common_gate, common_up, common_down, mixture)
```

```python
import jax
import jax.numpy as jnp
from jax import lax
from jax.sharding import PartitionSpec as P

EPSILON = 1e-05
ROUTED_SCALE = 2.5
BF16 = jnp.bfloat16
F32 = jnp.float32


def gather_tp(shard):
    length = lax.axis_size("tp")
    return lax.all_to_all(
        jnp.broadcast_to(shard[None], (length, *shard.shape)), "tp", 0, 0, tiled=True
    )


def mm(a, b):
    return jnp.dot(a, b, preferred_element_type=F32)


def mm_t(a, b):
    return lax.dot_general(a, b, (((1,), (1,)), ((), ())), preferred_element_type=F32)


def unpack_gate_up(parts):
    n, rows, both = parts.shape
    h = both // 2
    gate = parts[:, :, :h].transpose(1, 0, 2).reshape(rows, n * h)
    up = parts[:, :, h:].transpose(1, 0, 2).reshape(rows, n * h)
    return gate, up


def unpack_down(parts):
    n, src, half, both = parts.shape
    h = both // 2
    return (
        parts.reshape(n, src, half, 2, h).transpose(1, 3, 2, 0, 4).reshape(src * half * 2, n * h)
    )


def pack_down(down):
    half = down.shape[-2] // 2
    return jnp.concatenate([down[..., :half, :], down[..., half:, :]], axis=-1)


def on_device(
    tokens,
    routes,
    route_scores,
    norm_gain,
    expert_gate,
    expert_up,
    expert_down,
    shared_gate,
    shared_up,
    shared_down,
):
    n_fs, n_tp = lax.axis_size("fs"), lax.axis_size("tp")
    fs, tp = lax.axis_index("fs"), lax.axis_index("tp")
    rings = [list(range(c, n_fs, 2)) for c in range(2)]
    swap = [(i, i ^ 1) for i in range(n_fs)]
    rows_dev, feats = tokens.shape
    sub = rows_dev // n_tp
    width = feats * n_tp
    experts = expert_gate.shape[0]
    gain = norm_gain[:, None]
    hid = expert_gate.shape[2] * n_tp
    shared_hid = shared_gate.shape[1] * n_tp

    mine = lax.all_to_all(tokens.reshape(n_tp, sub, feats), "tp", 0, 0, tiled=True)
    values = mine.astype(F32)
    average = jnp.sum(values, axis=(0, 2)) / width
    meansq = jnp.sum(values * values, axis=(0, 2)) / width
    scale = lax.rsqrt(meansq - average * average + EPSILON)
    normed = ((values - average[None, :, None]) * scale[None, :, None]).astype(BF16)

    my_routes = lax.dynamic_slice_in_dim(routes, tp * sub, sub, 0)
    my_scores = lax.dynamic_slice_in_dim(route_scores, tp * sub, sub, 0)
    mix = my_scores / jnp.sum(my_scores, axis=1, keepdims=True) * ROUTED_SCALE
    named = my_routes[:, :, None] == jnp.arange(experts, dtype=jnp.int32)
    dense = jnp.sum(jnp.where(named, mix[:, :, None], 0.0), axis=1)
    high = dense.astype(BF16)
    low = (dense - high.astype(F32)).astype(BF16)
    payload = jnp.concatenate([*[normed[i] for i in range(n_tp)], high, low], axis=1)
    with jax.named_scope("tok_ag"):
        everyone = lax.all_gather(payload, "fs", axis=0, tiled=True, axis_index_groups=rings)

    gate_up = jnp.concatenate(
        [(expert_gate * gain).astype(BF16), (expert_up * gain).astype(BF16)], axis=2
    )
    with jax.named_scope("w_gu"):
        gate_up = lax.all_to_all(gate_up, "fs", 0, 0, tiled=True)
        gate, up = unpack_gate_up(gather_tp(gate_up.reshape(width, -1)))
    with jax.named_scope("w_dn"):
        down = lax.all_to_all(pack_down(expert_down.astype(BF16)), "fs", 0, 0, tiled=True)
        down = unpack_down(gather_tp(down))
    own = jnp.concatenate([gate, up, down], axis=1)
    other = lax.ppermute(own, "fs", swap)

    rows = everyone[:, :width]
    weights = everyone[:, width:].astype(F32)
    lanes = jnp.arange(2 * experts, dtype=jnp.int32) % experts
    partial = 0.0
    for w, e in ((own, fs), (other, fs ^ 1)):
        both = mm(rows, w[:, : 2 * hid]) * width**-0.5
        share = jnp.sum(jnp.where(lanes == e, weights, 0.0), axis=1, keepdims=True)
        hidden = (jax.nn.silu(both[:, :hid]) * both[:, hid:] * (share * hid**-0.5)).astype(BF16)
        partial = partial + mm_t(hidden, w[:, 2 * hid :])
    partial = partial.astype(BF16)

    packed = jnp.concatenate(
        [
            jnp.concatenate(
                [(shared_gate * gain).astype(BF16), (shared_up * gain).astype(BF16)], axis=1
            ),
            pack_down(shared_down.astype(BF16)),
        ],
        axis=0,
    )
    partial, packed, normed = lax.optimization_barrier((partial, packed, normed))
    with jax.named_scope("rs"):
        routed = lax.psum_scatter(
            partial, "fs", scatter_dimension=0, tiled=True, axis_index_groups=rings
        )
    local_rows = norm_gain.shape[0]
    with jax.named_scope("shared"):
        common = gather_tp_rows(lax.all_gather(packed, "fs", axis=0), local_rows)
        common_gate, common_up, common_down = common
        back = lax.all_to_all(normed, "tp", 0, 0, tiled=True).reshape(rows_dev, feats)
        part = jnp.concatenate([mm(back, common_gate), mm(back, common_up)], axis=1)
        part = (part * width**-0.5).astype(BF16)
        total = gather_tp(part).astype(F32).sum(axis=0)
        shared_hidden = (
            jax.nn.silu(total[:, :shared_hid]) * total[:, shared_hid:]
        ).astype(BF16)
        shared_part = mm_t(shared_hidden, common_down) * shared_hid**-0.5

    served = lax.dynamic_slice_in_dim(own, tp * feats, feats, 0)
    home = routed.reshape(sub, n_tp, feats).transpose(1, 0, 2)
    home = lax.all_to_all(home, "tp", 0, 0, tiled=True).reshape(rows_dev, feats)
    mixture = (shared_part + home.astype(F32)).astype(BF16)
    return (
        served[None, :, :hid],
        served[None, :, hid : 2 * hid],
        served[None, :, 2 * hid :],
        common_gate,
        common_up,
        common_down,
        mixture,
    )


def gather_tp_rows(packed, local_rows):
    n_tp = lax.axis_size("tp")
    n_fs = packed.shape[0]
    per = n_fs // n_tp
    split = packed.reshape(n_tp, per, *packed.shape[1:])
    split = lax.all_to_all(split, "tp", 0, 0, tiled=True)
    both = split[:, :, :local_rows].reshape(n_tp, per * local_rows, -1)
    gate, up = unpack_gate_up(both)
    return gate, up, unpack_down(split[:, :, local_rows:])


def solution(mesh):
    in_specs = (
        P(("grp", "fs"), "tp"),
        P(("grp", "fs"), None),
        P(("grp", "fs"), None),
        P("fs"),
        P(None, "fs", "tp"),
        P(None, "fs", "tp"),
        P(None, "fs", "tp"),
        P("fs", "tp"),
        P("fs", "tp"),
        P("fs", "tp"),
    )
    out_specs = (
        P(("grp", "fs"), "tp", None),
        P(("grp", "fs"), "tp", None),
        P(("grp", "fs"), "tp", None),
        P(("grp", "tp"), None),
        P(("grp", "tp"), None),
        P(("grp", "tp"), None),
        P(("grp", "fs"), "tp"),
    )
    return jax.shard_map(
        on_device, mesh=mesh, in_specs=in_specs, out_specs=out_specs, check_vma=False
    )
```

```python
import jax
import jax.numpy as jnp
from jax import lax
from jax.sharding import PartitionSpec as P

EPSILON = 1e-05
ROUTED_SCALE = 2.5
BF16 = jnp.bfloat16
F32 = jnp.float32


def broadcast_gather(shard, axis):
    length = lax.axis_size(axis)
    return lax.all_to_all(
        jnp.broadcast_to(shard[None], (length, *shard.shape)), axis, 0, 0, tiled=True
    )


def mm(a, b):
    return jnp.dot(a, b, preferred_element_type=F32)


def mm_t(a, b):
    return lax.dot_general(a, b, (((1,), (1,)), ((), ())), preferred_element_type=F32)


def unpack(parts, rows):
    n, src, _, both = parts.shape
    h = both // 2
    top, low = parts[:, :, :rows], parts[:, :, rows:]
    low = jnp.concatenate([low[..., :h], low[..., h:]], axis=2)
    return tuple(
        jnp.concatenate([a[i].reshape(src * rows, h) for i in range(n)], axis=1)
        for a in (top[..., :h], top[..., h:], low)
    )


def pack(gate, up, down):
    return jnp.concatenate([jnp.concatenate([gate, up], axis=-1), pack_down(down)], axis=-2)


def pack_down(down):
    half = down.shape[-2] // 2
    return jnp.concatenate([down[..., :half, :], down[..., half:, :]], axis=-1)


def on_device(
    tokens,
    routes,
    route_scores,
    norm_gain,
    expert_gate,
    expert_up,
    expert_down,
    shared_gate,
    shared_up,
    shared_down,
):
    n_fs, n_tp = lax.axis_size("fs"), lax.axis_size("tp")
    fs, tp = lax.axis_index("fs"), lax.axis_index("tp")
    rings = [list(range(c, n_fs, 2)) for c in range(2)]
    swap = [(i, i ^ 1) for i in range(n_fs)]
    rows_dev, feats = tokens.shape
    sub = rows_dev // n_tp
    width = feats * n_tp
    experts = expert_gate.shape[0]
    gain = norm_gain[:, None]
    hid = expert_gate.shape[2] * n_tp
    shared_hid = shared_gate.shape[1] * n_tp

    mine = lax.all_to_all(tokens.reshape(n_tp, sub, feats), "tp", 0, 0, tiled=True)
    values = mine.astype(F32)
    average = jnp.sum(values, axis=(0, 2)) / width
    meansq = jnp.sum(values * values, axis=(0, 2)) / width
    scale = lax.rsqrt(meansq - average * average + EPSILON)
    normed = ((values - average[None, :, None]) * scale[None, :, None]).astype(BF16)

    my_routes = lax.dynamic_slice_in_dim(routes, tp * sub, sub, 0)
    my_scores = lax.dynamic_slice_in_dim(route_scores, tp * sub, sub, 0)
    mix = my_scores / jnp.sum(my_scores, axis=1, keepdims=True) * ROUTED_SCALE
    named = my_routes[:, :, None] == jnp.arange(experts, dtype=jnp.int32)
    dense = jnp.sum(jnp.where(named, mix[:, :, None], 0.0), axis=1)
    high = dense.astype(BF16)
    low = (dense - high.astype(F32)).astype(BF16)
    payload = jnp.concatenate([*[normed[i] for i in range(n_tp)], high, low], axis=1)

    local_rows = norm_gain.shape[0]
    packed = pack(
        (expert_gate * gain).astype(BF16),
        (expert_up * gain).astype(BF16),
        expert_down.astype(BF16),
    )
    n_grp = lax.axis_size("grp")
    cut = packed.shape[1] // n_grp
    piece = lax.dynamic_slice_in_dim(packed, lax.axis_index("grp") * cut, cut, 1)
    payload, piece = lax.optimization_barrier((payload, piece))
    with jax.named_scope("tok_ag"):
        everyone = lax.all_gather(payload, "fs", axis=0, tiled=True, axis_index_groups=rings)
    with jax.named_scope("weights"):
        piece = lax.all_to_all(piece, "fs", 0, 0, tiled=True)
        pieces = broadcast_gather(piece, "grp")
        column = jnp.concatenate([pieces[i] for i in range(n_grp)], axis=1)
        gate, up, down = unpack(broadcast_gather(column, "tp"), local_rows)
    own = jnp.concatenate([gate, up, down], axis=1)
    other = lax.ppermute(own, "fs", swap)

    rows = everyone[:, :width]
    weights = everyone[:, width:].astype(F32)
    lanes = jnp.arange(2 * experts, dtype=jnp.int32) % experts
    partial = 0.0
    for w, e in ((own, fs), (other, fs ^ 1)):
        both = mm(rows, w[:, : 2 * hid]) * width**-0.5
        share = jnp.sum(jnp.where(lanes == e, weights, 0.0), axis=1, keepdims=True)
        hidden = (jax.nn.silu(both[:, :hid]) * both[:, hid:] * (share * hid**-0.5)).astype(BF16)
        partial = partial + mm_t(hidden, w[:, 2 * hid :])
    partial = partial.astype(BF16)

    packed = pack(
        (shared_gate * gain).astype(BF16),
        (shared_up * gain).astype(BF16),
        shared_down.astype(BF16),
    )
    partial, packed, normed = lax.optimization_barrier((partial, packed, normed))
    with jax.named_scope("rs"):
        routed = lax.psum_scatter(
            partial, "fs", scatter_dimension=0, tiled=True, axis_index_groups=rings
        )
    with jax.named_scope("shared"):
        common = lax.all_gather(packed, "fs", axis=0)
        common = common.reshape(n_tp, n_fs // n_tp, *common.shape[1:])
        common = lax.all_to_all(common, "tp", 0, 0, tiled=True)
        common_gate, common_up, common_down = unpack(common, local_rows)
        back = lax.all_to_all(normed, "tp", 0, 0, tiled=True).reshape(rows_dev, feats)
        part = jnp.concatenate([mm(back, common_gate), mm(back, common_up)], axis=1)
        part = (part * width**-0.5).astype(BF16)
        total = broadcast_gather(part, "tp").astype(F32).sum(axis=0)
        shared_hidden = (
            jax.nn.silu(total[:, :shared_hid]) * total[:, shared_hid:]
        ).astype(BF16)
        shared_part = mm_t(shared_hidden, common_down) * shared_hid**-0.5

    served = lax.dynamic_slice_in_dim(own, tp * feats, feats, 0)
    home = routed.reshape(sub, n_tp, feats).transpose(1, 0, 2)
    home = lax.all_to_all(home, "tp", 0, 0, tiled=True).reshape(rows_dev, feats)
    mixture = (shared_part + home.astype(F32)).astype(BF16)
    return (
        served[None, :, :hid],
        served[None, :, hid : 2 * hid],
        served[None, :, 2 * hid :],
        common_gate,
        common_up,
        common_down,
        mixture,
    )


def solution(mesh):
    in_specs = (
        P(("grp", "fs"), "tp"),
        P(("grp", "fs"), None),
        P(("grp", "fs"), None),
        P("fs"),
        P(None, "fs", "tp"),
        P(None, "fs", "tp"),
        P(None, "fs", "tp"),
        P("fs", "tp"),
        P("fs", "tp"),
        P("fs", "tp"),
    )
    out_specs = (
        P(("grp", "fs"), "tp", None),
        P(("grp", "fs"), "tp", None),
        P(("grp", "fs"), "tp", None),
        P(("grp", "tp"), None),
        P(("grp", "tp"), None),
        P(("grp", "tp"), None),
        P(("grp", "fs"), "tp"),
    )
    return jax.shard_map(
        on_device, mesh=mesh, in_specs=in_specs, out_specs=out_specs, check_vma=False
    )
```

```python
import jax
import jax.numpy as jnp
from jax import lax
from jax.sharding import PartitionSpec as P

EPSILON = 1e-05
ROUTED_SCALE = 2.5
BF16 = jnp.bfloat16
F32 = jnp.float32


def broadcast_gather(shard, axis):
    length = lax.axis_size(axis)
    return lax.all_to_all(
        jnp.broadcast_to(shard[None], (length, *shard.shape)), axis, 0, 0, tiled=True
    )


def mm(a, b):
    return jnp.dot(a, b, preferred_element_type=F32)


def mm_t(a, b):
    return lax.dot_general(a, b, (((1,), (1,)), ((), ())), preferred_element_type=F32)


def unpack(parts, rows):
    n, src, _, both = parts.shape
    h = both // 2
    top, low = parts[:, :, :rows], parts[:, :, rows:]
    low = jnp.concatenate([low[..., :h], low[..., h:]], axis=2)
    return tuple(
        jnp.concatenate([a[i].reshape(src * rows, h) for i in range(n)], axis=1)
        for a in (top[..., :h], top[..., h:], low)
    )


def pack(gate, up, down):
    return jnp.concatenate([jnp.concatenate([gate, up], axis=-1), pack_down(down)], axis=-2)


def pack_down(down):
    half = down.shape[-2] // 2
    return jnp.concatenate([down[..., :half, :], down[..., half:, :]], axis=-1)


def ring_sum(parts, n_fs, fs):
    n = n_fs // 2
    z = fs // 2
    half = n // 2
    ahead = [(i, (i + 2) % n_fs) for i in range(n_fs)]
    behind = [(i, (i - 2) % n_fs) for i in range(n_fs)]

    def part(k):
        return lax.dynamic_index_in_dim(parts, (z + k) % n, 0, keepdims=False)

    up, down = part(half), part(half + 1)
    for k in range(half - 1, -1, -1):
        up = lax.ppermute(up, "fs", ahead)
        if k < half - 1:
            down = lax.ppermute(down, "fs", behind)
        if k:
            up = up + part(k)
            if k < half - 1:
                down = down + part(n - k)
    return (up.astype(F32) + down.astype(F32) + part(0).astype(F32)).astype(BF16)


def on_device(
    tokens,
    routes,
    route_scores,
    norm_gain,
    expert_gate,
    expert_up,
    expert_down,
    shared_gate,
    shared_up,
    shared_down,
):
    n_fs, n_tp = lax.axis_size("fs"), lax.axis_size("tp")
    fs, tp = lax.axis_index("fs"), lax.axis_index("tp")
    rings = [list(range(c, n_fs, 2)) for c in range(2)]
    swap = [(i, i ^ 1) for i in range(n_fs)]
    rows_dev, feats = tokens.shape
    sub = rows_dev // n_tp
    width = feats * n_tp
    experts = expert_gate.shape[0]
    gain = norm_gain[:, None]
    hid = expert_gate.shape[2] * n_tp
    shared_hid = shared_gate.shape[1] * n_tp

    mine = lax.all_to_all(tokens.reshape(n_tp, sub, feats), "tp", 0, 0, tiled=True)
    values = mine.astype(F32)
    average = jnp.sum(values, axis=(0, 2)) / width
    meansq = jnp.sum(values * values, axis=(0, 2)) / width
    scale = lax.rsqrt(meansq - average * average + EPSILON)
    normed = ((values - average[None, :, None]) * scale[None, :, None]).astype(BF16)

    my_routes = lax.dynamic_slice_in_dim(routes, tp * sub, sub, 0)
    my_scores = lax.dynamic_slice_in_dim(route_scores, tp * sub, sub, 0)
    mix = my_scores / jnp.sum(my_scores, axis=1, keepdims=True) * ROUTED_SCALE
    named = my_routes[:, :, None] == jnp.arange(experts, dtype=jnp.int32)
    dense = jnp.sum(jnp.where(named, mix[:, :, None], 0.0), axis=1)
    high = dense.astype(BF16)
    low = (dense - high.astype(F32)).astype(BF16)
    payload = jnp.concatenate([*[normed[i] for i in range(n_tp)], high, low], axis=1)

    local_rows = norm_gain.shape[0]
    packed = pack(
        (expert_gate * gain).astype(BF16),
        (expert_up * gain).astype(BF16),
        expert_down.astype(BF16),
    )
    n_grp = lax.axis_size("grp")
    cut = packed.shape[1] // n_grp
    piece = lax.dynamic_slice_in_dim(packed, lax.axis_index("grp") * cut, cut, 1)
    shared_packed = pack(
        (shared_gate * gain).astype(BF16),
        (shared_up * gain).astype(BF16),
        shared_down.astype(BF16),
    )
    payload, piece, shared_packed = lax.optimization_barrier((payload, piece, shared_packed))
    with jax.named_scope("tok_ag"):
        everyone = lax.all_gather(payload, "fs", axis=0, tiled=True, axis_index_groups=rings)
    with jax.named_scope("weights"):
        piece = lax.all_to_all(piece, "fs", 0, 0, tiled=True)
        common = lax.all_gather(shared_packed, "fs", axis=0)
        piece, common = lax.optimization_barrier((piece, common))
        pieces = broadcast_gather(piece, "grp")
        column = jnp.concatenate([pieces[i] for i in range(n_grp)], axis=1)
        gate, up, down = unpack(broadcast_gather(column, "tp"), local_rows)
    own = jnp.concatenate([gate, up, down], axis=1)
    other = lax.ppermute(own, "fs", swap)

    with jax.named_scope("shared"):
        common = common.reshape(n_tp, n_fs // n_tp, *common.shape[1:])
        common = lax.all_to_all(common, "tp", 0, 0, tiled=True)
        common_gate, common_up, common_down = unpack(common, local_rows)
        back = lax.all_to_all(normed, "tp", 0, 0, tiled=True).reshape(rows_dev, feats)
        part = jnp.concatenate([mm(back, common_gate), mm(back, common_up)], axis=1)
        part = (part * width**-0.5).astype(BF16)
        total = broadcast_gather(part, "tp").astype(F32).sum(axis=0)

    everyone, total = lax.optimization_barrier((everyone, total))
    rows = everyone[:, :width]
    weights = everyone[:, width:].astype(F32)
    lanes = jnp.arange(2 * experts, dtype=jnp.int32) % experts
    hiddens = []
    for w, e in ((own, fs), (other, fs ^ 1)):
        both = mm(rows, w[:, : 2 * hid]) * width**-0.5
        share = jnp.sum(jnp.where(lanes == e, weights, 0.0), axis=1, keepdims=True)
        hiddens.append(
            (jax.nn.silu(both[:, :hid]) * both[:, hid:] * (share * hid**-0.5)).astype(BF16)
        )

    def outputs(low, high):
        return (
            mm_t(hiddens[0], own[low:high, 2 * hid :]) + mm_t(hiddens[1], other[low:high, 2 * hid :])
        ).astype(BF16)

    edge = width * 5 // 8
    first = outputs(0, edge)
    with jax.named_scope("rs"):
        routed = lax.psum_scatter(
            first, "fs", scatter_dimension=0, tiled=True, axis_index_groups=rings
        )
    second = outputs(edge, width).reshape(n_fs // 2, sub, width - edge)
    with jax.named_scope("ring"):
        beside = ring_sum(second, n_fs, fs)
    routed = jnp.concatenate([routed, beside], axis=1)
    with jax.named_scope("shared_out"):
        shared_hidden = (
            jax.nn.silu(total[:, :shared_hid]) * total[:, shared_hid:]
        ).astype(BF16)
        shared_part = mm_t(shared_hidden, common_down) * shared_hid**-0.5

    served = lax.dynamic_slice_in_dim(own, tp * feats, feats, 0)
    home = routed.reshape(sub, n_tp, feats).transpose(1, 0, 2)
    home = lax.all_to_all(home, "tp", 0, 0, tiled=True).reshape(rows_dev, feats)
    mixture = (shared_part + home.astype(F32)).astype(BF16)
    return (
        served[None, :, :hid],
        served[None, :, hid : 2 * hid],
        served[None, :, 2 * hid :],
        common_gate,
        common_up,
        common_down,
        mixture,
    )


def solution(mesh):
    in_specs = (
        P(("grp", "fs"), "tp"),
        P(("grp", "fs"), None),
        P(("grp", "fs"), None),
        P("fs"),
        P(None, "fs", "tp"),
        P(None, "fs", "tp"),
        P(None, "fs", "tp"),
        P("fs", "tp"),
        P("fs", "tp"),
        P("fs", "tp"),
    )
    out_specs = (
        P(("grp", "fs"), "tp", None),
        P(("grp", "fs"), "tp", None),
        P(("grp", "fs"), "tp", None),
        P(("grp", "tp"), None),
        P(("grp", "tp"), None),
        P(("grp", "tp"), None),
        P(("grp", "fs"), "tp"),
    )
    return jax.shard_map(
        on_device, mesh=mesh, in_specs=in_specs, out_specs=out_specs, check_vma=False
    )
```

```python
import jax
import jax.numpy as jnp
from jax import lax
from jax.sharding import PartitionSpec as P

EPSILON = 1e-05
ROUTED_SCALE = 2.5
BF16 = jnp.bfloat16
F32 = jnp.float32


def broadcast_gather(shard, axis):
    length = lax.axis_size(axis)
    return lax.all_to_all(
        jnp.broadcast_to(shard[None], (length, *shard.shape)), axis, 0, 0, tiled=True
    )


def mm(a, b):
    return jnp.dot(a, b, preferred_element_type=F32)


def mm_t(a, b):
    return lax.dot_general(a, b, (((1,), (1,)), ((), ())), preferred_element_type=F32)


def unpack(parts, rows):
    n, src, _, both = parts.shape
    h = both // 2
    top, low = parts[:, :, :rows], parts[:, :, rows:]
    low = jnp.concatenate([low[..., :h], low[..., h:]], axis=2)
    return tuple(
        jnp.concatenate([a[i].reshape(src * rows, h) for i in range(n)], axis=1)
        for a in (top[..., :h], top[..., h:], low)
    )


def pack(gate, up, down):
    return jnp.concatenate([jnp.concatenate([gate, up], axis=-1), pack_down(down)], axis=-2)


def pack_down(down):
    half = down.shape[-2] // 2
    return jnp.concatenate([down[..., :half, :], down[..., half:, :]], axis=-1)


def on_device(
    tokens,
    routes,
    route_scores,
    norm_gain,
    expert_gate,
    expert_up,
    expert_down,
    shared_gate,
    shared_up,
    shared_down,
):
    n_fs, n_tp = lax.axis_size("fs"), lax.axis_size("tp")
    fs, tp = lax.axis_index("fs"), lax.axis_index("tp")
    rings = [list(range(c, n_fs, 2)) for c in range(2)]
    swap = [(i, i ^ 1) for i in range(n_fs)]
    rows_dev, feats = tokens.shape
    sub = rows_dev // n_tp
    width = feats * n_tp
    experts = expert_gate.shape[0]
    gain = norm_gain[:, None]
    hid = expert_gate.shape[2] * n_tp
    shared_hid = shared_gate.shape[1] * n_tp

    mine = lax.all_to_all(tokens.reshape(n_tp, sub, feats), "tp", 0, 0, tiled=True)
    values = mine.astype(F32)
    average = jnp.sum(values, axis=(0, 2)) / width
    meansq = jnp.sum(values * values, axis=(0, 2)) / width
    scale = lax.rsqrt(meansq - average * average + EPSILON)
    normed = ((values - average[None, :, None]) * scale[None, :, None]).astype(BF16)

    my_routes = lax.dynamic_slice_in_dim(routes, tp * sub, sub, 0)
    my_scores = lax.dynamic_slice_in_dim(route_scores, tp * sub, sub, 0)
    mix = my_scores / jnp.sum(my_scores, axis=1, keepdims=True) * ROUTED_SCALE
    named = my_routes[:, :, None] == jnp.arange(experts, dtype=jnp.int32)
    dense = jnp.sum(jnp.where(named, mix[:, :, None], 0.0), axis=1)
    high = dense.astype(BF16)
    low = (dense - high.astype(F32)).astype(BF16)
    payload = jnp.concatenate([*[normed[i] for i in range(n_tp)], high, low], axis=1)

    local_rows = norm_gain.shape[0]
    packed = pack(
        (expert_gate * gain).astype(BF16),
        (expert_up * gain).astype(BF16),
        expert_down.astype(BF16),
    )
    n_grp = lax.axis_size("grp")
    cut = packed.shape[1] // n_grp
    piece = lax.dynamic_slice_in_dim(packed, lax.axis_index("grp") * cut, cut, 1)
    payload, piece = lax.optimization_barrier((payload, piece))
    with jax.named_scope("tok_ag"):
        everyone = lax.all_gather(payload, "fs", axis=0, tiled=True, axis_index_groups=rings)
    with jax.named_scope("weights"):
        piece = lax.all_to_all(piece, "fs", 0, 0, tiled=True)
        pieces = broadcast_gather(piece, "grp")
        column = jnp.concatenate([pieces[i] for i in range(n_grp)], axis=1)
        gate, up, down = unpack(broadcast_gather(column, "tp"), local_rows)
    own = jnp.concatenate([gate, up, down], axis=1)
    other = lax.ppermute(own, "fs", swap)

    inward = jnp.concatenate([own[:, : 2 * hid], other[:, : 2 * hid]], axis=1)
    outward = jnp.concatenate([own[:, 2 * hid :], other[:, 2 * hid :]], axis=1)
    everyone, inward, outward = lax.optimization_barrier((everyone, inward, outward))
    rows = everyone[:, :width]
    weights = everyone[:, width:].astype(F32)
    lanes = jnp.arange(2 * experts, dtype=jnp.int32) % experts
    both = mm(rows, inward) * width**-0.5
    hiddens = []
    for i, e in enumerate((fs, fs ^ 1)):
        gated, raised = (both[:, k * hid : (k + 1) * hid] for k in (2 * i, 2 * i + 1))
        share = jnp.sum(jnp.where(lanes == e, weights, 0.0), axis=1, keepdims=True)
        hiddens.append((jax.nn.silu(gated) * raised * (share * hid**-0.5)).astype(BF16))
    partial = mm_t(jnp.concatenate(hiddens, axis=1), outward)
    partial = partial.astype(BF16)

    packed = pack(
        (shared_gate * gain).astype(BF16),
        (shared_up * gain).astype(BF16),
        shared_down.astype(BF16),
    )
    partial, packed, normed = lax.optimization_barrier((partial, packed, normed))
    with jax.named_scope("rs"):
        routed = lax.psum_scatter(
            partial, "fs", scatter_dimension=0, tiled=True, axis_index_groups=rings
        )
    with jax.named_scope("shared"):
        common = lax.all_gather(packed, "fs", axis=0)
        common = common.reshape(n_tp, n_fs // n_tp, *common.shape[1:])
        common = lax.all_to_all(common, "tp", 0, 0, tiled=True)
        common_gate, common_up, common_down = unpack(common, local_rows)
        back = lax.all_to_all(normed, "tp", 0, 0, tiled=True).reshape(rows_dev, feats)
        part = jnp.concatenate([mm(back, common_gate), mm(back, common_up)], axis=1)
        part = (part * width**-0.5).astype(BF16)
        total = broadcast_gather(part, "tp").astype(F32).sum(axis=0)
        shared_hidden = (
            jax.nn.silu(total[:, :shared_hid]) * total[:, shared_hid:]
        ).astype(BF16)
        shared_part = mm_t(shared_hidden, common_down) * shared_hid**-0.5

    served = lax.dynamic_slice_in_dim(own, tp * feats, feats, 0)
    home = routed.reshape(sub, n_tp, feats).transpose(1, 0, 2)
    home = lax.all_to_all(home, "tp", 0, 0, tiled=True).reshape(rows_dev, feats)
    mixture = (shared_part + home.astype(F32)).astype(BF16)
    return (
        served[None, :, :hid],
        served[None, :, hid : 2 * hid],
        served[None, :, 2 * hid :],
        common_gate,
        common_up,
        common_down,
        mixture,
    )


def solution(mesh):
    in_specs = (
        P(("grp", "fs"), "tp"),
        P(("grp", "fs"), None),
        P(("grp", "fs"), None),
        P("fs"),
        P(None, "fs", "tp"),
        P(None, "fs", "tp"),
        P(None, "fs", "tp"),
        P("fs", "tp"),
        P("fs", "tp"),
        P("fs", "tp"),
    )
    out_specs = (
        P(("grp", "fs"), "tp", None),
        P(("grp", "fs"), "tp", None),
        P(("grp", "fs"), "tp", None),
        P(("grp", "tp"), None),
        P(("grp", "tp"), None),
        P(("grp", "tp"), None),
        P(("grp", "fs"), "tp"),
    )
    return jax.shard_map(
        on_device, mesh=mesh, in_specs=in_specs, out_specs=out_specs, check_vma=False
    )
```
